32 devices in a mesh: sp: 16 (over z, y, x), tp: 2 (over core).
Axes of the slice: x: 2, y: 2, z: 4, core: 2. Of those that a mesh axis runs over, the one named last changes fastest.
Arguments:
- tokens: bfloat16 [2048, 2048], P(('sp', 'tp')), may hold values from -6 to 6
- input_norm_gain: float32 [2048], replicated, may hold values from 0.1 to 1.9
- differential_query: bfloat16 [2048, 1024], P(None, 'tp'), may hold values from -0.176776695 to 0.176776695, as said below
- differential_key: bfloat16 [2048, 1024], P(None, 'tp'), may hold values from -0.176776695 to 0.176776695, as said below
- differential_value: bfloat16 [2048, 1024], P(None, 'tp'), may hold values from -0.125 to 0.125
- query_norm_gain: float32 [64], replicated, may hold values from 1.15 to 5
- key_norm_gain: float32 [64], replicated, may hold values from 1.15 to 5
- second_map_weight: float32 [8], P('tp'), may hold values from 0.3 to 0.8
- differential_norm_gain: float32 [128], replicated, may hold values from 0.1 to 1.9
- linear_query: bfloat16 [2048, 512], P(None, 'tp'), may hold values from -0.125 to 0.125
- linear_key: bfloat16 [2048, 512], P(None, 'tp'), may hold values from -0.125 to 0.125
- linear_value: bfloat16 [2048, 1024], P(None, 'tp'), may hold values from -0.125 to 0.125
- linear_output_gate: bfloat16 [2048, 1024], P(None, 'tp'), may hold values from -0.125 to 0.125
- forget_down_factor: bfloat16 [2048, 32], replicated, may hold values from -0.125 to 0.125
- forget_up_factor: bfloat16 [32, 512], P(None, 'tp'), may hold values from -2.109375 to 2.109375
- forget_bias: float32 [512], P('tp'), may hold values from -0.5 to 10
- extra_shrinkage_exponent: float32 [2048, 8], P('sp', 'tp'), may hold values from -1.5 to 0
- linear_norm_gain: float32 [128], replicated, may hold values from 0.1 to 1.9
- differential_output_rows: bfloat16 [1024, 2048], P('tp'), may hold values from -0.125 to 0.125
- linear_output_rows: bfloat16 [1024, 2048], P('tp'), may hold values from -0.125 to 0.125
Outputs:
- layer_out: bfloat16 [2048, 2048], P(('sp', 'tp'))
The draws below stay inside these ranges and needn't reach their ends.
Inputs may be any that keep to these rules, and one draw needn't show every extreme that they name: `differential_query`: independent entries of scale one over sqrt(2048). `differential_key`: entries of scale one over sqrt(2048).
All inputs are finite; a program needn't handle non-finite values.
Results may differ from the reference program's by a relative error of at most 0.015.
Values may be sent and summed in bfloat16 or wider, within the bound.
A program may use at most 64 MiB of HBM per device.

```python
import math
import jax
import jax.numpy as jnp
from jax import lax

D = 2048
DA_HEADS = 8
HEAD = 64
VDIM = 128
RECURRENT_LANES = 8
RECURRENT_DIM = 64
GLA_DV = 128
RANK = 32
BLOCK = 64
TOK_DEV = 128
SEQUENCE_LENGTH = 2048
N_SP = 16
N_TP = 2


def attn_pair(key):
    base_part = jnp.clip(jax.random.normal(jax.random.fold_in(key, 11), (D, DA_HEADS * 2 * HEAD), jnp.float32), -6.0, 6.0)
    noise_part = jnp.clip(jax.random.normal(jax.random.fold_in(key, 12), (D, DA_HEADS * 2 * HEAD), jnp.float32), -6.0, 6.0)
    key_weight = noise_part
    return (base_part * D ** (-0.5), key_weight * D ** (-0.5))


def draw_differential_query(key, part):
    return attn_pair(key)[0].astype(jnp.bfloat16)


def draw_differential_key(key, part):
    return attn_pair(key)[1].astype(jnp.bfloat16)


def gain_draw(key):
    values = jax.random.uniform(key, (HEAD,), jnp.float32, 1.15, 1.45)
    return values


def draw_query_norm_gain(key, part):
    return gain_draw(jax.random.fold_in(key, 31))


def draw_key_norm_gain(key, part):
    return gain_draw(jax.random.fold_in(key, 32))


def draw_forget_bias(key, part):
    ranking = jax.random.permutation(jax.random.fold_in(key, 41), RECURRENT_LANES)
    fast_heads = ranking < RECURRENT_LANES // 2
    fast_bias = jax.random.uniform(jax.random.fold_in(key, 42), (RECURRENT_LANES, RECURRENT_DIM), jnp.float32, -0.5, 0.5)
    slow_bias = jax.random.uniform(jax.random.fold_in(key, 43), (RECURRENT_LANES, RECURRENT_DIM), jnp.float32, 8.0, 10.0)
    return jnp.where(fast_heads[:, None], fast_bias, slow_bias).reshape(RECURRENT_LANES * RECURRENT_DIM)


def draw_extra_shrinkage_exponent(key, part):
    block_total = SEQUENCE_LENGTH // TOK_DEV
    block_rates = jnp.exp(jax.random.uniform(jax.random.fold_in(key, 51), (block_total, 1, RECURRENT_LANES), jnp.float32, math.log(0.2), math.log(1.0))) / SEQUENCE_LENGTH
    baseline_rate = -jnp.broadcast_to(block_rates, (block_total, TOK_DEV, RECURRENT_LANES)).reshape(SEQUENCE_LENGTH, RECURRENT_LANES)
    spike_positions = jax.random.randint(jax.random.fold_in(key, 52), (3,), 0, SEQUENCE_LENGTH)
    spike_drops = jnp.log(jax.random.uniform(jax.random.fold_in(key, 53), (3, RECURRENT_LANES), jnp.float32, 0.5, 0.8))
    spike_hits = (jnp.arange(SEQUENCE_LENGTH, dtype=jnp.int32)[:, None] == spike_positions[None, :]).astype(jnp.float32)
    return baseline_rate + jnp.dot(spike_hits, spike_drops)


def level_of(rng, dims, pieces, smallest, largest):
    gain = 1.0
    for position, parts in pieces:
        steps = jax.random.uniform(jax.random.fold_in(jax.random.fold_in(rng, 6), position), (parts,), jnp.float32, smallest / len(pieces), largest / len(pieces))
        gain = gain * jnp.repeat(jnp.exp(steps), dims[position] // parts).reshape((-1,) + (1,) * (len(dims) - 1 - position))
    return gain


def centred(key, dims, scale, most, split=(), kind=jnp.bfloat16):
    values = jax.random.normal(key, dims, jnp.float32) * scale
    if len(split) > 0:
        values = level_of(key, dims, split, -0.22, 0.18) * values
    return jnp.clip(values, min=-most, max=most).astype(kind)


def setup_inputs(seed: int = 0) -> dict:
    arg_keys = jax.random.split(jax.random.key(seed), 21)
    tokens = centred(arg_keys[0], (SEQUENCE_LENGTH, D), 1.0, 6.0, ((0, 32),))
    input_norm_gain = jnp.clip(1.0 + 0.18 * jax.random.normal(arg_keys[1], (D,), jnp.float32), 0.1, 1.9)
    differential_query = draw_differential_query(jax.random.fold_in(arg_keys[20], 71), 0)
    differential_key = draw_differential_key(jax.random.fold_in(arg_keys[20], 71), 0)
    differential_value = centred(arg_keys[4], (D, DA_HEADS * VDIM), D ** -0.5, 0.125, ((1, 2),))
    query_norm_gain = draw_query_norm_gain(jax.random.fold_in(arg_keys[20], 71), 0)
    key_norm_gain = draw_key_norm_gain(jax.random.fold_in(arg_keys[20], 71), 0)
    second_map_weight = jnp.clip(0.3 + 0.5 * jax.random.uniform(arg_keys[7], (DA_HEADS,), jnp.float32) ** level_of(arg_keys[7], (DA_HEADS,), ((0, 2),), -0.2, 0.2), 0.3, 0.8)
    differential_norm_gain = jnp.clip(1.0 + 0.18 * jax.random.normal(arg_keys[8], (VDIM,), jnp.float32), 0.1, 1.9)
    linear_query = centred(arg_keys[9], (D, RECURRENT_LANES * RECURRENT_DIM), D ** -0.5, 0.125, ((1, 2),))
    linear_key = centred(arg_keys[10], (D, RECURRENT_LANES * RECURRENT_DIM), D ** -0.5, 0.125, ((1, 2),))
    linear_value = centred(arg_keys[11], (D, RECURRENT_LANES * GLA_DV), D ** -0.5, 0.125, ((1, 2),))
    linear_output_gate = centred(arg_keys[12], (D, RECURRENT_LANES * GLA_DV), D ** -0.5, 0.125, ((1, 2),))
    forget_down_factor = centred(arg_keys[13], (D, RANK), D ** -0.5, 0.125)
    forget_up_factor = centred(arg_keys[14], (RANK, RECURRENT_LANES * RECURRENT_DIM), (2.0 * RANK ** -0.5), 2.109375, ((1, 2),))
    forget_bias = draw_forget_bias(jax.random.fold_in(arg_keys[20], 71), 0)
    extra_shrinkage_exponent = draw_extra_shrinkage_exponent(jax.random.fold_in(arg_keys[20], 71), 0)
    linear_norm_gain = jnp.clip(1.0 + 0.18 * jax.random.normal(arg_keys[17], (GLA_DV,), jnp.float32), 0.1, 1.9)
    differential_output_rows = centred(arg_keys[18], (DA_HEADS * VDIM, D), (DA_HEADS * VDIM + RECURRENT_LANES * GLA_DV) ** -0.5, 0.125, ((0, 2),))
    linear_output_rows = centred(arg_keys[19], (RECURRENT_LANES * GLA_DV, D), (DA_HEADS * VDIM + RECURRENT_LANES * GLA_DV) ** -0.5, 0.125, ((0, 2),))
    return dict(tokens=tokens, input_norm_gain=input_norm_gain, differential_query=differential_query, differential_key=differential_key, differential_value=differential_value, query_norm_gain=query_norm_gain, key_norm_gain=key_norm_gain, second_map_weight=second_map_weight, differential_norm_gain=differential_norm_gain, linear_query=linear_query, linear_key=linear_key, linear_value=linear_value, linear_output_gate=linear_output_gate, forget_down_factor=forget_down_factor, forget_up_factor=forget_up_factor, forget_bias=forget_bias, extra_shrinkage_exponent=extra_shrinkage_exponent, linear_norm_gain=linear_norm_gain, differential_output_rows=differential_output_rows, linear_output_rows=linear_output_rows)


RMS_EPS = 1e-06
SOFTMAX_DIVISOR = 16.0
OUT_SCALE = 0.8
HIGHEST = lax.Precision.HIGHEST

def rms_scale(values, scale_gain):
    mean_sq = lax.optimization_barrier(jnp.mean(values * values, axis=-1, keepdims=True))
    return values * lax.rsqrt(mean_sq + RMS_EPS) * scale_gain

def attention_reference(query_norm, key_norm, value_rows, second_map_weight):
    positions = jnp.arange(SEQUENCE_LENGTH, dtype=jnp.int32)

    def one_head(inputs):
        query_head, key_head, value_head, lambda_value = inputs
        key_float = key_head.astype(jnp.float32)

        def one_block(first_row):
            query_block = lax.dynamic_slice_in_dim(query_head, first_row, TOK_DEV, 0).astype(jnp.float32)
            scores = jnp.einsum('tmd,kmd->mtk', query_block, key_float) * HEAD ** (-0.5)
            query_pos = first_row + jnp.arange(TOK_DEV, dtype=jnp.int32)
            causal = positions[None, :] <= query_pos[:, None]
            scores = jnp.where(causal[None], scores, -jnp.inf)
            row_peak = lax.optimization_barrier(jnp.max(scores, axis=-1, keepdims=True))
            weights = jnp.exp(scores - row_peak)
            totals = lax.optimization_barrier(jnp.sum(weights, axis=-1))
            first_map = jnp.dot(weights[0].astype(jnp.bfloat16), value_head, preferred_element_type=jnp.float32) / totals[0][:, None]
            second = jnp.dot(weights[1].astype(jnp.bfloat16), value_head, preferred_element_type=jnp.float32) / totals[1][:, None]
            return first_map - lambda_value * second
        starts = jnp.arange(N_SP, dtype=jnp.int32) * TOK_DEV
        return lax.map(one_block, starts).reshape(SEQUENCE_LENGTH, VDIM)
    return lax.map(one_head, (query_norm.transpose(1, 0, 2, 3), key_norm.transpose(1, 0, 2, 3), value_rows.transpose(1, 0, 2), second_map_weight))

def chain_reference(queries, keys_rows, values_rows, shrinkage_exponent):
    blocks = SEQUENCE_LENGTH // BLOCK

    def blockify(array):
        return array.reshape(blocks, BLOCK, RECURRENT_LANES, array.shape[-1])
    causal = jnp.tril(jnp.ones((BLOCK, BLOCK), dtype=bool))

    def step_block(carried, inputs):
        query_block, key_block, value_block, decay_block = inputs
        log_cum = jnp.cumsum(decay_block, axis=0)
        inter = jnp.einsum('thd,hde->the', query_block * jnp.exp(log_cum), carried, precision=HIGHEST)
        differences = log_cum[:, None] - log_cum[None, :]
        decay_table = jnp.exp(jnp.where(causal[:, :, None, None], differences, -jnp.inf))
        inner_scores = jnp.einsum('thd,shd,tshd->hts', query_block, key_block, decay_table, precision=HIGHEST)
        intra = jnp.einsum('hts,she->the', inner_scores, value_block, precision=HIGHEST)
        log_last = log_cum[-1]
        key_end = key_block * jnp.exp(log_last[None] - log_cum)
        carried = carried * jnp.exp(log_last)[..., None] + jnp.einsum('thd,the->hde', key_end, value_block, precision=HIGHEST)
        return (carried, inter + intra)
    state_zero = jnp.zeros((RECURRENT_LANES, RECURRENT_DIM, GLA_DV), jnp.float32)
    _, outputs = lax.scan(step_block, state_zero, (blockify(queries), blockify(keys_rows), blockify(values_rows), blockify(shrinkage_exponent)))
    return outputs.reshape(SEQUENCE_LENGTH, RECURRENT_LANES, GLA_DV)

def reference(tokens, input_norm_gain, differential_query, differential_key, differential_value, query_norm_gain, key_norm_gain, second_map_weight, differential_norm_gain, linear_query, linear_key, linear_value, linear_output_gate, forget_down_factor, forget_up_factor, forget_bias, extra_shrinkage_exponent, linear_norm_gain, differential_output_rows, linear_output_rows):
    normed = rms_scale(tokens.astype(jnp.float32), input_norm_gain).astype(jnp.bfloat16)

    def project(matrix):
        return jnp.dot(normed, matrix, preferred_element_type=jnp.float32).astype(jnp.bfloat16)
    query_norm = rms_scale(project(differential_query).astype(jnp.float32).reshape(SEQUENCE_LENGTH, DA_HEADS, 2, HEAD), query_norm_gain).astype(jnp.bfloat16)
    key_norm = rms_scale(project(differential_key).astype(jnp.float32).reshape(SEQUENCE_LENGTH, DA_HEADS, 2, HEAD), key_norm_gain).astype(jnp.bfloat16)
    value_rows = project(differential_value).reshape(SEQUENCE_LENGTH, DA_HEADS, VDIM)
    attn_maps = attention_reference(query_norm, key_norm, value_rows, second_map_weight)
    attn_out = (rms_scale(attn_maps, differential_norm_gain) * OUT_SCALE).transpose(1, 0, 2).reshape(SEQUENCE_LENGTH, DA_HEADS * VDIM).astype(jnp.bfloat16)
    queries = project(linear_query).astype(jnp.float32).reshape(SEQUENCE_LENGTH, RECURRENT_LANES, RECURRENT_DIM) * RECURRENT_DIM ** (-0.5)
    keys_rows = project(linear_key).astype(jnp.float32).reshape(SEQUENCE_LENGTH, RECURRENT_LANES, RECURRENT_DIM)
    values_rows = project(linear_value).astype(jnp.float32).reshape(SEQUENCE_LENGTH, RECURRENT_LANES, GLA_DV)
    gated = jax.nn.silu(project(linear_output_gate).astype(jnp.float32)).reshape(SEQUENCE_LENGTH, RECURRENT_LANES, GLA_DV)
    low_rank = project(forget_down_factor)
    sigmoid_preactivation = jnp.dot(low_rank, forget_up_factor, preferred_element_type=jnp.float32) + forget_bias
    shrinkage_exponent = jax.nn.log_sigmoid(sigmoid_preactivation).reshape(SEQUENCE_LENGTH, RECURRENT_LANES, RECURRENT_DIM) / SOFTMAX_DIVISOR + extra_shrinkage_exponent[:, :, None]
    chain_full = chain_reference(queries, keys_rows, values_rows, shrinkage_exponent)
    chain_out = (rms_scale(chain_full, linear_norm_gain) * gated).reshape(SEQUENCE_LENGTH, RECURRENT_LANES * GLA_DV).astype(jnp.bfloat16)
    attn_width = DA_HEADS // N_TP * VDIM
    chain_width = RECURRENT_LANES // N_TP * GLA_DV
    summed = jnp.zeros((SEQUENCE_LENGTH, D), jnp.float32)
    for group_index in range(N_TP):
        attn_cols = attn_out[:, group_index * attn_width:(group_index + 1) * attn_width]
        chain_cols = chain_out[:, group_index * chain_width:(group_index + 1) * chain_width]
        group_term = jnp.dot(attn_cols, differential_output_rows[group_index * attn_width:(group_index + 1) * attn_width], preferred_element_type=jnp.float32)
        group_term = group_term + jnp.dot(chain_cols, linear_output_rows[group_index * chain_width:(group_index + 1) * chain_width], preferred_element_type=jnp.float32)
        summed = summed + lax.optimization_barrier(group_term.astype(jnp.bfloat16)).astype(jnp.float32)
    return summed.astype(jnp.bfloat16)
```

```python
import functools

import jax
import jax.numpy as jnp
import numpy as np
from jax import lax
from jax.experimental import pallas as pl
from jax.experimental.pallas import tpu as pltpu
from jax.sharding import PartitionSpec as P

HEAD = 64
VDIM = 128
RECURRENT_DIM = 64
LANES = 128
RMS_EPS = 1e-06
OUT_SCALE = 0.8
MESH = pl.DeviceIdType.MESH
F32 = jnp.float32
BF16 = jnp.bfloat16


def dot(a, b):
    return jnp.dot(a, b, preferred_element_type=F32)


def dot_t(a, b):
    return lax.dot_general(a, b, (((1,), (1,)), ((), ())), preferred_element_type=F32)


def decay_tables(rows):
    levels = rows.bit_length() - 1
    t = np.arange(rows)[:, None]
    r = np.arange(rows)[None, :]
    parts = []
    for level in range(levels):
        h = 1 << level
        mid = (t // (2 * h)) * 2 * h + h - 1
        upper = (t // h) % 2 == 1
        parts.append(np.where(upper, (r > mid) & (r <= t), (r > t) & (r <= mid)))
    parts.append(r <= t)
    parts.append(r > t)
    pair_level = np.full((rows, rows), -1, np.int32)
    for level in range(levels):
        pair_level[((t ^ r) >> level == 1) & (t > r)] = level
    pair_level[t == r] = levels
    return np.concatenate(parts, 0).astype(np.float32), pair_level, levels


def body(
    cfg,
    tokens, gain, wq, wk, wv, wlq, wlk, wlv, wlg, wdown, up, bias, extra, qgain, kgain, lam,
    dgain, lgain, wo1, wo2, table, pair_level,
    out,
    xbuf, xn, wbuf, wl, ebuf, proj, plin, logs, kv, q2, acc, peak, total, wo, qd, inner, states,
    pre, pref_in, pref_out, obuf, mix, terms, got,
    w_sem, xs_in, xs_tp, x_recv, es, er, kv_send, kv_recv, st_send, st_recv, a_send, a_recv,
    c_send, c_recv, t_send, t_recv,
):
    G, N, T, r, R, S, D, LW, levels = cfg
    sp = lax.axis_index("sp")
    t = lax.axis_index("tp")
    o = lax.div(sp, G)
    i = lax.rem(sp, G)
    wide = LW == LANES
    pairs = LANES // RECURRENT_DIM

    col = pl.multiple_of(i * LANES, LANES)
    lcol = pl.multiple_of(lax.div(i, pairs) * LANES, LANES) if wide else 0
    loads = []
    for n, w in enumerate((wq, wk, wv, wlv, wlg)):
        loads.append(
            pltpu.make_async_copy(
                w.at[:, pl.ds(col, LANES)], wbuf.at[:, pl.ds(n * LANES, LANES)], w_sem.at[n]
            )
        )
    for n, w in enumerate((wlq, wlk)):
        src = w.at[:, pl.ds(lcol, LW)] if wide else w
        dst = wbuf.at[:, pl.ds((5 + n) * LANES, LANES)] if wide else wl.at[n]
        loads.append(pltpu.make_async_copy(src, dst, w_sem.at[5 + n]))
    for copy in loads:
        copy.start()
    wo_loads = [
        pltpu.make_async_copy(w, wo.at[n], w_sem.at[7 + n]) for n, w in enumerate((wo1, wo2))
    ]
    for copy in wo_loads:
        copy.start()

    def peer(d):
        return o * G + lax.rem(i + d, G)

    def source(d):
        return lax.rem(i - d + G, G)

    def tpeer(k):
        return lax.rem(t + k, T)

    barrier = pltpu.get_barrier_semaphore()
    for d in range(G):
        for k in range(T):
            if d or k:
                pl.semaphore_signal(
                    barrier, inc=1, device_id=(peer(d), tpeer(k)), device_id_type=MESH
                )

    @pl.when(o > 0)
    def _():
        pl.semaphore_signal(barrier, inc=1, device_id=(sp - G, t), device_id_type=MESH)

    @pl.when(o < N - 1)
    def _():
        pl.semaphore_signal(barrier, inc=1, device_id=(sp + G, t), device_id_type=MESH)

    inside = (o > 0) & (o < N - 1)

    @pl.when(inside)
    def _():
        pl.semaphore_wait(barrier, G * T + 1)

    @pl.when(jnp.logical_not(inside))
    def _():
        pl.semaphore_wait(barrier, G * T if N > 1 else G * T - 1)

    def remote(src, dst, ss, rs, where):
        return pltpu.make_async_remote_copy(
            src_ref=src, dst_ref=dst, send_sem=ss, recv_sem=rs, device_id=where,
            device_id_type=MESH,
        )

    own = i * T + t
    sends = []
    for k in range(1, T):
        sends.append(
            remote(tokens, xbuf.at[own], xs_tp.at[k], x_recv.at[own], (sp, tpeer(k)))
        )
    for d in range(1, G):
        sends.append(remote(tokens, xbuf.at[own], xs_in.at[d], x_recv.at[own], (peer(d), t)))
    for d in range(1, G):
        sends.append(remote(extra, ebuf.at[i], es.at[d], er.at[i], (peer(d), t)))
    for copy in sends:
        copy.start()
    xbuf[own] = tokens[...]
    ebuf[i] = extra[...]

    def arrival(slot):
        remote(
            tokens, xbuf.at[slot], xs_in.at[0], x_recv.at[slot], (peer(1) if G > 1 else sp, tpeer(1))
        ).wait_recv()

    def forward(d):
        j = source(d)
        slot = j * T + t
        arrival(slot)
        for k in range(1, T):
            copy = remote(
                xbuf.at[slot], xbuf.at[slot], xs_tp.at[d * T + k], x_recv.at[slot], (sp, tpeer(k))
            )
            copy.start()
            sends.append(copy)

    lane = lax.broadcasted_iota(jnp.int32, (1, LANES), 1)
    low_half = lane < HEAD

    def map_norm(values, map_gain):
        sq = values * values
        first = jnp.sum(jnp.where(low_half, sq, 0.0), axis=-1, keepdims=True)
        second = jnp.sum(jnp.where(low_half, 0.0, sq), axis=-1, keepdims=True)
        scale = jnp.where(
            low_half,
            lax.rsqrt(first * (1.0 / HEAD) + RMS_EPS),
            lax.rsqrt(second * (1.0 / HEAD) + RMS_EPS),
        )
        return values * scale * map_gain

    def project(d):
        j = source(d)
        for k in range(1, T):
            arrival(j * T + tpeer(k))
        if d > 0:
            remote(extra, ebuf.at[j], es.at[0], er.at[j], (peer(1), t)).wait_recv()
        for c in range(T):
            x = xbuf[j * T + c].astype(F32)
            ms = jnp.mean(x * x, axis=-1, keepdims=True)
            xn[pl.ds(c * r, r), :] = (x * lax.rsqrt(ms + RMS_EPS) * gain[...]).astype(BF16)
        if d == 0:
            for copy in loads:
                copy.wait()
        x = xn[...]
        rows = pl.ds(pl.multiple_of(j * R, R), R)
        proj_block = dot(x, wbuf[...]).astype(BF16)
        qn = map_norm(proj_block[:, 0:LANES].astype(F32), qgain[...]).astype(BF16) * HEAD ** (-0.5)
        qn = qn.astype(BF16)
        zero = jnp.zeros_like(qn)
        q2[0, rows, :] = jnp.where(low_half, qn, zero)
        q2[1, rows, :] = jnp.where(low_half, zero, qn)
        kn = map_norm(proj_block[:, LANES : 2 * LANES].astype(F32), kgain[...]).astype(BF16)
        kv[o, rows, 0:LANES] = kn
        kv[o, rows, LANES : 2 * LANES] = proj_block[:, 2 * LANES : 3 * LANES]
        proj[rows, :] = proj_block[:, 3 * LANES : 5 * LANES]
        if wide:
            mine = lax.div(lane, RECURRENT_DIM) == lax.rem(i, pairs)
            for n in range(2):
                part = proj_block[:, (5 + n) * LANES : (6 + n) * LANES]
                plin[n, rows, :] = jnp.where(mine, part, jnp.zeros_like(part))
        else:
            for n in range(2):
                plin[n, rows, :] = dot(x, wl[n]).astype(BF16)
        low = dot(x, wdown[...]).astype(BF16)
        lsl = pl.ds(lcol, LW)
        pre_act = dot(low, up[:, lsl]) + bias[:, lsl]
        log_sig = jnp.minimum(pre_act, 0.0) - jnp.log1p(jnp.exp(-jnp.abs(pre_act)))
        turned = ebuf[j].T
        head_lane = lax.broadcasted_iota(jnp.int32, (1, turned.shape[1]), 1)
        add = jnp.sum(jnp.where(head_lane == i, turned, 0.0), axis=1, keepdims=True)
        logs[rows, :] = log_sig * (1.0 / 16.0) + add

    if G > 1:
        forward(1)
    for d in range(G):
        if 0 < d and d + 1 < G:
            forward(d + 1)
        elif d == 0 and G > 1:
            pass
        project(d)

    def kv_copy(slot):
        return remote(
            kv.at[slot], kv.at[slot], kv_send.at[slot], kv_recv.at[slot], (sp + G, t)
        )

    @pl.when(o < N - 1)
    def _():
        kv_copy(o).start()

    level_of = pair_level[...]
    states[...] = jnp.zeros_like(states)
    pre[...] = jnp.zeros_like(pre)

    def chain_block(b, _):
        rows = pl.ds(pl.multiple_of(b * R, R), R)
        la = logs[rows, :]
        hi = la.astype(BF16)
        lo = (la - hi.astype(F32)).astype(BF16)
        q = plin[0, rows, :].astype(F32) * RECURRENT_DIM ** (-0.5)
        k = plin[1, rows, :].astype(F32)
        v = proj[rows, 0:LANES]
        sums = dot(table[...], hi) + dot(table[...], lo)
        scores = jnp.where(level_of == levels, dot_t(q.astype(BF16), k.astype(BF16)), 0.0)
        for level in range(levels):
            e = jnp.exp(sums[level * R : (level + 1) * R])
            part = dot_t((q * e).astype(BF16), (k * e).astype(BF16))
            scores = scores + jnp.where(level_of == level, part, 0.0)
        inner[rows, :] = dot(scores.astype(BF16), v)
        cum = sums[levels * R : (levels + 1) * R]
        suffix = sums[(levels + 1) * R : (levels + 2) * R]
        qd[rows, :] = (q * jnp.exp(cum)).astype(BF16)
        k_end = (k * jnp.exp(suffix)).astype(BF16)
        last = cum[R - 1 : R, :]
        vt = v.astype(F32).T.astype(BF16)
        states[b + 1] = states[b] * jnp.exp(last) + dot(vt, k_end)
        pre[b + 1] = pre[b] + last
        return 0

    lax.fori_loop(0, G, chain_block, 0)

    def prefix_copy():
        return remote(
            pref_out.at[...], pref_in.at[...], st_send.at[0], st_recv.at[0], (sp + G, t)
        )

    TQ = min(2 * LANES, S)

    def attend(slot, first):
        k = kv.at[slot]

        def tile(j, _):
            m = lax.div(j, S // TQ)
            start = pl.multiple_of(lax.rem(j, S // TQ) * TQ, TQ)
            rows = pl.ds(start, TQ)
            s = dot_t(q2[m, rows, :], k[:, 0:LANES])
            if first:
                u = lax.broadcasted_iota(jnp.int32, (TQ, S), 1)
                tt = lax.broadcasted_iota(jnp.int32, (TQ, S), 0) + start
                s = jnp.where(u <= tt, s, -1e30)
                new = jnp.max(s, axis=-1, keepdims=True)
                p = jnp.exp(s - new)
                total[m, rows, :] = jnp.broadcast_to(
                    jnp.sum(p, axis=-1, keepdims=True), (TQ, LANES)
                )
                acc[m, rows, :] = dot(p.astype(BF16), k[:, LANES : 2 * LANES])
                peak[m, rows, :] = jnp.broadcast_to(new, (TQ, LANES))
            else:
                old = peak[m, rows, :]
                new = jnp.maximum(old, jnp.max(s, axis=-1, keepdims=True))
                p = jnp.exp(s - new[:, 0:1])
                factor = jnp.exp(old - new)
                total[m, rows, :] = total[m, rows, :] * factor + jnp.sum(
                    p, axis=-1, keepdims=True
                )
                acc[m, rows, :] = acc[m, rows, :] * factor + dot(
                    p.astype(BF16), k[:, LANES : 2 * LANES]
                )
                peak[m, rows, :] = new
            return 0

        lax.fori_loop(0, 2 * S // TQ, tile, 0)

    attend(o, True)

    def take(slot):
        kv_copy(slot).wait_recv()

        @pl.when(o < N - 1)
        def _():
            kv_copy(slot).start()

    @pl.when(o > 0)
    def _():
        take(o - 1)
        prefix_copy().wait_recv()

    @pl.when(o == 0)
    def _():
        pref_in[...] = jnp.zeros_like(pref_in)

    carried = pref_in[...]

    @pl.when(o < N - 1)
    def _():
        pref_out[...] = carried * jnp.exp(pre[G]) + states[G]
        prefix_copy().start()

    def chain_finish(b, _):
        rows = pl.ds(pl.multiple_of(b * R, R), R)
        state = (states[b] + pref_in[...] * jnp.exp(pre[b])).astype(BF16)
        full = inner[rows, :] + dot_t(qd[rows, :], state)
        gate = proj[rows, LANES : 2 * LANES].astype(F32)
        ms = jnp.mean(full * full, axis=-1, keepdims=True)
        gate = gate / (1.0 + jnp.exp(-gate))
        obuf[1, b] = (full * lax.rsqrt(ms + RMS_EPS) * lgain[...] * gate).astype(BF16)
        return 0

    lax.fori_loop(0, G, chain_finish, 0)

    def give(n, ss, rs):
        copies = []
        for d in range(1, G):
            j = lax.rem(i + d, G)
            copies.append(
                remote(obuf.at[n, j], mix.at[n, i], ss.at[d], rs.at[i], (peer(d), t))
            )
        for copy in copies:
            copy.start()
        mix[n, i] = obuf[n, i]
        return copies

    def collect(n, ss, rs):
        for d in range(1, G):
            j = source(d)
            remote(obuf.at[n, j], mix.at[n, j], ss.at[0], rs.at[j], (peer(1), t)).wait_recv()

    sends += give(1, c_send, c_recv)

    def earlier(s, _):
        slot = o - s

        @pl.when(s > 1)
        def _():
            take(slot)

        attend(slot, False)
        return 0

    lax.fori_loop(1, o + 1, earlier, 0)

    weight = lam[i]

    def attn_finish(b, _):
        rows = pl.ds(pl.multiple_of(b * R, R), R)
        diff = acc[0, rows, :] / total[0, rows, :] - weight * (
            acc[1, rows, :] / total[1, rows, :]
        )
        ms = jnp.mean(diff * diff, axis=-1, keepdims=True)
        obuf[0, b] = (diff * lax.rsqrt(ms + RMS_EPS) * dgain[...] * OUT_SCALE).astype(BF16)
        return 0

    lax.fori_loop(0, G, attn_finish, 0)
    sends += give(0, a_send, a_recv)
    for copy in wo_loads:
        copy.wait()
    collect(1, c_send, c_recv)
    chain_mix = jnp.concatenate([mix[1, j] for j in range(G)], axis=1)
    chain_part = dot(chain_mix, wo[1])
    collect(0, a_send, a_recv)
    attn_mix = jnp.concatenate([mix[0, j] for j in range(G)], axis=1)
    term = (dot(attn_mix, wo[0]) + chain_part).astype(BF16)
    for c in range(T):
        terms[c] = term[c * r : (c + 1) * r]
    for k in range(1, T):
        copy = remote(terms.at[tpeer(k)], got.at[t], t_send.at[k], t_recv.at[t], (sp, tpeer(k)))
        copy.start()
        sends.append(copy)
    summed = terms[t].astype(F32)
    for k in range(1, T):
        c = tpeer(k)
        remote(terms.at[c], got.at[c], t_send.at[0], t_recv.at[c], (sp, c)).wait_recv()
        summed = summed + got[c].astype(F32)
    out[...] = summed.astype(BF16)

    for copy in sends:
        copy.wait_send()

    @pl.when(o < N - 1)
    def _():
        prefix_copy().wait_send()

        def drain(s, _):
            kv_copy(s).wait_send()
            return 0

        lax.fori_loop(0, o + 1, drain, 0)


def per_device(
    tokens, input_norm_gain, differential_query, differential_key, differential_value,
    query_norm_gain, key_norm_gain, second_map_weight, differential_norm_gain, linear_query,
    linear_key, linear_value, linear_output_gate, forget_down_factor, forget_up_factor,
    forget_bias, extra_shrinkage_exponent, linear_norm_gain, differential_output_rows,
    linear_output_rows,
):
    sp_size, T = lax.axis_size("sp"), lax.axis_size("tp")
    G = second_map_weight.shape[0]
    r, D = tokens.shape
    R = r * T
    N = sp_size // G
    S = G * R
    LW = min(LANES, G * RECURRENT_DIM)
    table, pair_level, levels = decay_tables(R)
    cfg = (G, N, T, r, R, S, D, LW, levels)
    row = lambda a: a.reshape(1, -1)
    extra = jnp.pad(extra_shrinkage_exponent.T, ((0, -G % 8), (0, 0)))
    vmem = pl.BlockSpec(memory_space=pltpu.VMEM)
    smem = pl.BlockSpec(memory_space=pltpu.SMEM)
    anys = pl.BlockSpec(memory_space=pl.ANY)
    wide = LW == LANES
    dma = pltpu.SemaphoreType.DMA
    return pl.pallas_call(
        functools.partial(body, cfg),
        out_shape=jax.ShapeDtypeStruct((r, D), BF16),
        in_specs=[vmem] * 2 + [anys] * 7 + [vmem] * 6 + [smem] + [vmem] * 2 + [anys] * 2 + [vmem] * 2,
        out_specs=vmem,
        scratch_shapes=[
            pltpu.VMEM((G * T, r, D), BF16),
            pltpu.VMEM((R, D), BF16),
            pltpu.VMEM((D, (7 if wide else 5) * LANES), BF16),
            pltpu.VMEM((2, 16, LANES) if wide else (2, D, LW), BF16),
            pltpu.VMEM((G,) + extra.shape, F32),
            pltpu.VMEM((S, 2 * LANES), BF16),
            pltpu.VMEM((2, S, LW), BF16),
            pltpu.VMEM((S, LW), F32),
            pltpu.VMEM((N, S, 2 * LANES), BF16),
            pltpu.VMEM((2, S, LANES), BF16),
            pltpu.VMEM((2, S, LANES), F32),
            pltpu.VMEM((2, S, LANES), F32),
            pltpu.VMEM((2, S, LANES), F32),
            pltpu.VMEM((2,) + differential_output_rows.shape, BF16),
            pltpu.VMEM((S, LW), BF16),
            pltpu.VMEM((S, LANES), F32),
            pltpu.VMEM((G + 1, VDIM, LW), F32),
            pltpu.VMEM((G + 1, 1, LW), F32),
            pltpu.VMEM((VDIM, LW), F32),
            pltpu.VMEM((VDIM, LW), F32),
            pltpu.VMEM((2, G, R, LANES), BF16),
            pltpu.VMEM((2, G, R, LANES), BF16),
            pltpu.VMEM((T, r, D), BF16),
            pltpu.VMEM((T, r, D), BF16),
            dma((9,)),
            dma((G,)),
            dma((G * T,)),
            dma((G * T,)),
            dma((G,)),
            dma((G,)),
            dma((N,)),
            dma((N,)),
            dma((1,)),
            dma((1,)),
            dma((G,)),
            dma((G,)),
            dma((G,)),
            dma((G,)),
            dma((T,)),
            dma((T,)),
        ],
        compiler_params=pltpu.CompilerParams(
            collective_id=0, has_side_effects=True, vmem_limit_bytes=60 * 1024 * 1024
        ),
        name="layer",
    )(
        tokens, row(input_norm_gain), differential_query, differential_key, differential_value,
        linear_query, linear_key, linear_value, linear_output_gate, forget_down_factor,
        forget_up_factor, row(forget_bias), extra,
        row(jnp.tile(query_norm_gain, 2)), row(jnp.tile(key_norm_gain, 2)), second_map_weight,
        row(differential_norm_gain), row(linear_norm_gain), differential_output_rows,
        linear_output_rows, jnp.asarray(table, BF16), jnp.asarray(pair_level),
    )


def solution(mesh):
    placed = (
        P(("sp", "tp"), None),
        P(),
        P(None, "tp"),
        P(None, "tp"),
        P(None, "tp"),
        P(),
        P(),
        P("tp"),
        P(),
        P(None, "tp"),
        P(None, "tp"),
        P(None, "tp"),
        P(None, "tp"),
        P(),
        P(None, "tp"),
        P("tp"),
        P("sp", "tp"),
        P(),
        P("tp", None),
        P("tp", None),
    )
    return jax.shard_map(
        per_device, mesh=mesh, in_specs=placed, out_specs=P(("sp", "tp"), None), check_vma=False
    )
```

```python
import functools

import jax
import jax.numpy as jnp
import numpy as np
from jax import lax
from jax.experimental import pallas as pl
from jax.experimental.pallas import tpu as pltpu
from jax.sharding import PartitionSpec as P

HEAD = 64
VDIM = 128
RECURRENT_DIM = 64
LANES = 128
RMS_EPS = 1e-06
OUT_SCALE = 0.8
MESH = pl.DeviceIdType.MESH
F32 = jnp.float32
BF16 = jnp.bfloat16


def dot(a, b):
    return jnp.dot(a, b, preferred_element_type=F32)


def dot_t(a, b):
    return lax.dot_general(a, b, (((1,), (1,)), ((), ())), preferred_element_type=F32)


def decay_tables(rows):
    levels = rows.bit_length() - 1
    t = np.arange(rows)[:, None]
    r = np.arange(rows)[None, :]
    parts = []
    for level in range(levels):
        h = 1 << level
        mid = (t // (2 * h)) * 2 * h + h - 1
        upper = (t // h) % 2 == 1
        parts.append(np.where(upper, (r > mid) & (r <= t), (r > t) & (r <= mid)))
    parts.append(r <= t)
    parts.append(r > t)
    pair_level = np.full((rows, rows), -1, np.int32)
    for level in range(levels):
        pair_level[((t ^ r) >> level == 1) & (t > r)] = level
    pair_level[t == r] = levels
    return np.concatenate(parts, 0).astype(np.float32), pair_level, levels


def body(
    cfg,
    tokens, gain, wq, wk, wv, wlq, wlk, wlv, wlg, wdown, up, bias, extra, qgain, kgain, lam,
    dgain, lgain, wo1, wo2, table, pair_level,
    out,
    xbuf, xn, wbuf, wl, ebuf, proj, plin, logs, kv, q2, acc, peak, total, wo, qd, inner, states,
    pre, pref_in, pref_out, obuf, mix, terms, got,
    w_sem, xs_in, xs_tp, x_recv, es, er, kv_send, kv_recv, st_send, st_recv, a_send, a_recv,
    c_send, c_recv, t_send, t_recv,
):
    G, N, T, r, R, S, D, LW, levels = cfg
    sp = lax.axis_index("sp")
    t = lax.axis_index("tp")
    o = lax.div(sp, G)
    i = lax.rem(sp, G)
    wide = LW == LANES
    pairs = LANES // RECURRENT_DIM

    col = pl.multiple_of(i * LANES, LANES)
    lcol = pl.multiple_of(lax.div(i, pairs) * LANES, LANES) if wide else 0
    loads = []
    for n, w in enumerate((wq, wk, wv, wlv, wlg)):
        loads.append(
            pltpu.make_async_copy(
                w.at[:, pl.ds(col, LANES)], wbuf.at[:, pl.ds(n * LANES, LANES)], w_sem.at[n]
            )
        )
    for n, w in enumerate((wlq, wlk)):
        src = w.at[:, pl.ds(lcol, LW)] if wide else w
        dst = wbuf.at[:, pl.ds((5 + n) * LANES, LANES)] if wide else wl.at[n]
        loads.append(pltpu.make_async_copy(src, dst, w_sem.at[5 + n]))
    for copy in loads:
        copy.start()
    wo_loads = [
        pltpu.make_async_copy(w, wo.at[n], w_sem.at[7 + n]) for n, w in enumerate((wo1, wo2))
    ]

    def peer(d):
        return o * G + lax.rem(i + d, G)

    def source(d):
        return lax.rem(i - d + G, G)

    def tpeer(k):
        return lax.rem(t + k, T)

    barrier = pltpu.get_barrier_semaphore()
    for d in range(G):
        for k in range(T):
            if d or k:
                pl.semaphore_signal(
                    barrier, inc=1, device_id=(peer(d), tpeer(k)), device_id_type=MESH
                )

    @pl.when(o > 0)
    def _():
        pl.semaphore_signal(barrier, inc=1, device_id=(sp - G, t), device_id_type=MESH)

    @pl.when(o < N - 1)
    def _():
        pl.semaphore_signal(barrier, inc=1, device_id=(sp + G, t), device_id_type=MESH)

    inside = (o > 0) & (o < N - 1)

    @pl.when(inside)
    def _():
        pl.semaphore_wait(barrier, G * T + 1)

    @pl.when(jnp.logical_not(inside))
    def _():
        pl.semaphore_wait(barrier, G * T if N > 1 else G * T - 1)

    def remote(src, dst, ss, rs, where):
        return pltpu.make_async_remote_copy(
            src_ref=src, dst_ref=dst, send_sem=ss, recv_sem=rs, device_id=where,
            device_id_type=MESH,
        )

    own = i * T + t
    sends = []
    for k in range(1, T):
        sends.append(
            remote(tokens, xbuf.at[own], xs_tp.at[k], x_recv.at[own], (sp, tpeer(k)))
        )
    for d in range(1, G):
        sends.append(remote(tokens, xbuf.at[own], xs_in.at[d], x_recv.at[own], (peer(d), t)))
    for d in range(1, G):
        sends.append(remote(extra, ebuf.at[i], es.at[d], er.at[i], (peer(d), t)))
    for copy in sends:
        copy.start()
    xbuf[own] = tokens[...]
    ebuf[i] = extra[...]

    def arrival(slot):
        remote(
            tokens, xbuf.at[slot], xs_in.at[0], x_recv.at[slot], (peer(1) if G > 1 else sp, tpeer(1))
        ).wait_recv()

    def forward(d):
        j = source(d)
        slot = j * T + t
        arrival(slot)
        for k in range(1, T):
            copy = remote(
                xbuf.at[slot], xbuf.at[slot], xs_tp.at[d * T + k], x_recv.at[slot], (sp, tpeer(k))
            )
            copy.start()
            sends.append(copy)

    lane = lax.broadcasted_iota(jnp.int32, (1, LANES), 1)
    low_half = lane < HEAD

    qg = jnp.concatenate([qgain[...], qgain[...]], axis=1)
    kg = jnp.concatenate([kgain[...], kgain[...]], axis=1)

    def map_norm(values, map_gain):
        sq = values * values
        first = jnp.sum(jnp.where(low_half, sq, 0.0), axis=-1, keepdims=True)
        second = jnp.sum(jnp.where(low_half, 0.0, sq), axis=-1, keepdims=True)
        scale = jnp.where(
            low_half,
            lax.rsqrt(first * (1.0 / HEAD) + RMS_EPS),
            lax.rsqrt(second * (1.0 / HEAD) + RMS_EPS),
        )
        return values * scale * map_gain

    def project(d):
        j = source(d)
        for k in range(1, T):
            arrival(j * T + tpeer(k))
        if d > 0:
            remote(extra, ebuf.at[j], es.at[0], er.at[j], (peer(1), t)).wait_recv()
        for c in range(T):
            x = xbuf[j * T + c].astype(F32)
            ms = jnp.mean(x * x, axis=-1, keepdims=True)
            xn[pl.ds(c * r, r), :] = (x * lax.rsqrt(ms + RMS_EPS) * gain[...]).astype(BF16)
        if d == 0:
            for copy in loads:
                copy.wait()
            for copy in wo_loads:
                copy.start()
        x = xn[...]
        rows = pl.ds(pl.multiple_of(j * R, R), R)
        proj_block = dot(x, wbuf[...]).astype(BF16)
        qn = map_norm(proj_block[:, 0:LANES].astype(F32), qg).astype(BF16) * HEAD ** (-0.5)
        qn = qn.astype(BF16)
        zero = jnp.zeros_like(qn)
        q2[0, rows, :] = jnp.where(low_half, qn, zero)
        q2[1, rows, :] = jnp.where(low_half, zero, qn)
        kn = map_norm(proj_block[:, LANES : 2 * LANES].astype(F32), kg).astype(BF16)
        kv[o, rows, 0:LANES] = kn
        kv[o, rows, LANES : 2 * LANES] = proj_block[:, 2 * LANES : 3 * LANES]
        proj[rows, :] = proj_block[:, 3 * LANES : 5 * LANES]
        if wide:
            mine = lax.div(lane, RECURRENT_DIM) == lax.rem(i, pairs)
            for n in range(2):
                part = proj_block[:, (5 + n) * LANES : (6 + n) * LANES]
                plin[n, rows, :] = jnp.where(mine, part, jnp.zeros_like(part))
        else:
            for n in range(2):
                plin[n, rows, :] = dot(x, wl[n]).astype(BF16)
        low = dot_t(x, wdown[...]).astype(BF16)
        lsl = pl.ds(lcol, LW)
        pre_act = dot(low, up[:, lsl]) + bias[:, lsl]
        log_sig = jnp.minimum(pre_act, 0.0) - jnp.log1p(jnp.exp(-jnp.abs(pre_act)))
        turned = jnp.concatenate([ebuf[j]] + [jnp.zeros((-G % 8, R), F32)] * (G % 8 > 0), axis=0).T
        head_lane = lax.broadcasted_iota(jnp.int32, (1, turned.shape[1]), 1)
        add = jnp.sum(jnp.where(head_lane == i, turned, 0.0), axis=1, keepdims=True)
        logs[rows, :] = log_sig * (1.0 / 16.0) + add

    def kv_copy(slot, j):
        part = kv.at[slot, pl.ds(pl.multiple_of(j * R, R), R)]
        n = slot * G + j
        return remote(part, part, kv_send.at[n], kv_recv.at[n], (sp + G, t))

    def relay(step):
        def one(s, _):
            slot, j = o - s, source(step - s)
            kv_copy(slot, j).wait_recv()

            @pl.when(o < N - 1)
            def _():
                kv_copy(slot, j).start()

            return 0

        lax.fori_loop(jnp.maximum(1, step - G + 1), jnp.minimum(o, step) + 1, one, 0)

    for d in range(G):
        if 0 < d and d + 1 < G:
            forward(d + 1)
        project(d)

        @pl.when(o < N - 1)
        def _():
            kv_copy(o, source(d)).start()

        if d == 0 and G > 1:
            forward(1)
        relay(d)

    level_of = pair_level[...]
    states[...] = jnp.zeros_like(states)
    pre[...] = jnp.zeros_like(pre)

    def chain_block(b, _):
        rows = pl.ds(pl.multiple_of(b * R, R), R)
        la = logs[rows, :]
        hi = la.astype(BF16)
        lo = (la - hi.astype(F32)).astype(BF16)
        q = plin[0, rows, :].astype(F32) * RECURRENT_DIM ** (-0.5)
        k = plin[1, rows, :].astype(F32)
        v = proj[rows, 0:LANES]
        sums = dot(table[...], hi) + dot(table[...], lo)
        scores = jnp.where(level_of == levels, dot_t(q.astype(BF16), k.astype(BF16)), 0.0)
        for level in range(levels):
            e = jnp.exp(sums[level * R : (level + 1) * R])
            part = dot_t((q * e).astype(BF16), (k * e).astype(BF16))
            scores = scores + jnp.where(level_of == level, part, 0.0)
        inner[rows, :] = dot(scores.astype(BF16), v)
        cum = sums[levels * R : (levels + 1) * R]
        suffix = sums[(levels + 1) * R : (levels + 2) * R]
        qd[rows, :] = (q * jnp.exp(cum)).astype(BF16)
        k_end = (k * jnp.exp(suffix)).astype(BF16)
        last = cum[R - 1 : R, :]
        vt = v.astype(F32).T.astype(BF16)
        states[b + 1] = states[b] * jnp.exp(last) + dot(vt, k_end)
        pre[b + 1] = pre[b] + last
        return 0

    lax.fori_loop(0, G, chain_block, 0)

    def prefix_copy():
        return remote(
            pref_out.at[...], pref_in.at[...], st_send.at[0], st_recv.at[0], (sp + G, t)
        )

    TQ = min(2 * LANES, S)

    def attend(slot, first):
        k = kv.at[slot]

        def tile(j, _):
            m = lax.div(j, S // TQ)
            start = pl.multiple_of(lax.rem(j, S // TQ) * TQ, TQ)
            rows = pl.ds(start, TQ)
            s = dot_t(q2[m, rows, :], k[:, 0:LANES])
            if first:
                u = lax.broadcasted_iota(jnp.int32, (TQ, S), 1)
                tt = lax.broadcasted_iota(jnp.int32, (TQ, S), 0) + start
                s = jnp.where(u <= tt, s, -1e30)
                new = jnp.max(s, axis=-1, keepdims=True)
                p = jnp.exp(s - new)
                total[m, rows, :] = jnp.broadcast_to(
                    jnp.sum(p, axis=-1, keepdims=True), (TQ, LANES)
                )
                acc[m, rows, :] = dot(p.astype(BF16), k[:, LANES : 2 * LANES])
                peak[m, rows, :] = jnp.broadcast_to(new, (TQ, LANES))
            else:
                old = peak[m, rows, :]
                new = jnp.maximum(old, jnp.max(s, axis=-1, keepdims=True))
                p = jnp.exp(s - new[:, 0:1])
                factor = jnp.exp(old - new)
                total[m, rows, :] = total[m, rows, :] * factor + jnp.sum(
                    p, axis=-1, keepdims=True
                )
                acc[m, rows, :] = acc[m, rows, :] * factor + dot(
                    p.astype(BF16), k[:, LANES : 2 * LANES]
                )
                peak[m, rows, :] = new
            return 0

        lax.fori_loop(0, 2 * S // TQ, tile, 0)

    def give(n, ss, rs):
        copies = []
        for d in range(1, G):
            j = lax.rem(i + d, G)
            copies.append(
                remote(obuf.at[n, j], mix.at[n, i], ss.at[d], rs.at[i], (peer(d), t))
            )
        return copies

    def collect(n, ss, rs):
        for d in range(1, G):
            j = source(d)
            remote(obuf.at[n, j], mix.at[n, j], ss.at[0], rs.at[j], (peer(1), t)).wait_recv()

    def chain_finish(b, _):
        rows = pl.ds(pl.multiple_of(b * R, R), R)
        state = (states[b] + pref_in[...] * jnp.exp(pre[b])).astype(BF16)
        full = inner[rows, :] + dot_t(qd[rows, :], state)
        gate = proj[rows, LANES : 2 * LANES].astype(F32)
        ms = jnp.mean(full * full, axis=-1, keepdims=True)
        gate = gate / (1.0 + jnp.exp(-gate))
        obuf[1, b] = (full * lax.rsqrt(ms + RMS_EPS) * lgain[...] * gate).astype(BF16)
        return 0

    def chain_tail():
        @pl.when(o < N - 1)
        def _():
            pref_out[...] = pref_in[...] * jnp.exp(pre[G]) + states[G]
            prefix_copy().start()

        lax.fori_loop(0, G, chain_finish, 0)
        for copy in give(1, c_send, c_recv):
            copy.start()
        mix[1, i] = obuf[1, i]

    @pl.when(o == 0)
    def _():
        pref_in[...] = jnp.zeros_like(pref_in)
        chain_tail()

    relay(G)
    attend(o, True)

    def earlier(s, _):
        @pl.when(s > 1)
        def _():
            relay(s + G - 1)

        @pl.when(s == o)
        def _():
            prefix_copy().wait_recv()
            chain_tail()

        attend(o - s, False)
        return 0

    lax.fori_loop(1, o + 1, earlier, 0)
    sends += give(1, c_send, c_recv)

    weight = lam[i]

    def attn_finish(b, _):
        rows = pl.ds(pl.multiple_of(b * R, R), R)
        diff = acc[0, rows, :] / total[0, rows, :] - weight * (
            acc[1, rows, :] / total[1, rows, :]
        )
        ms = jnp.mean(diff * diff, axis=-1, keepdims=True)
        obuf[0, b] = (diff * lax.rsqrt(ms + RMS_EPS) * dgain[...] * OUT_SCALE).astype(BF16)
        return 0

    lax.fori_loop(0, G, attn_finish, 0)
    attn_sends = give(0, a_send, a_recv)
    for copy in attn_sends:
        copy.start()
    sends += attn_sends
    mix[0, i] = obuf[0, i]
    for copy in wo_loads:
        copy.wait()
    collect(1, c_send, c_recv)
    chain_mix = jnp.concatenate([mix[1, j] for j in range(G)], axis=1)
    chain_part = dot(chain_mix, wo[1])
    collect(0, a_send, a_recv)
    attn_mix = jnp.concatenate([mix[0, j] for j in range(G)], axis=1)
    term = (dot(attn_mix, wo[0]) + chain_part).astype(BF16)
    for c in range(T):
        terms[c] = term[c * r : (c + 1) * r]
    for k in range(1, T):
        copy = remote(terms.at[tpeer(k)], got.at[t], t_send.at[k], t_recv.at[t], (sp, tpeer(k)))
        copy.start()
        sends.append(copy)
    summed = terms[t].astype(F32)
    for k in range(1, T):
        c = tpeer(k)
        remote(terms.at[c], got.at[c], t_send.at[0], t_recv.at[c], (sp, c)).wait_recv()
        summed = summed + got[c].astype(F32)
    out[...] = summed.astype(BF16)

    for copy in sends:
        copy.wait_send()

    @pl.when(o < N - 1)
    def _():
        prefix_copy().wait_send()

        def drain(s, _):
            for j in range(G):
                kv_copy(s, j).wait_send()
            return 0

        lax.fori_loop(0, o + 1, drain, 0)


def per_device(
    tokens, input_norm_gain, differential_query, differential_key, differential_value,
    query_norm_gain, key_norm_gain, second_map_weight, differential_norm_gain, linear_query,
    linear_key, linear_value, linear_output_gate, forget_down_factor, forget_up_factor,
    forget_bias, extra_shrinkage_exponent, linear_norm_gain, differential_output_rows,
    linear_output_rows,
):
    sp_size, T = lax.axis_size("sp"), lax.axis_size("tp")
    G = second_map_weight.shape[0]
    r, D = tokens.shape
    R = r * T
    N = sp_size // G
    S = G * R
    LW = min(LANES, G * RECURRENT_DIM)
    table, pair_level, levels = decay_tables(R)
    cfg = (G, N, T, r, R, S, D, LW, levels)
    row = lambda a: a.reshape(1, -1)
    extra = extra_shrinkage_exponent.T
    vmem = pl.BlockSpec(memory_space=pltpu.VMEM)
    smem = pl.BlockSpec(memory_space=pltpu.SMEM)
    anys = pl.BlockSpec(memory_space=pl.ANY)
    wide = LW == LANES
    dma = pltpu.SemaphoreType.DMA
    return pl.pallas_call(
        functools.partial(body, cfg),
        out_shape=jax.ShapeDtypeStruct((r, D), BF16),
        in_specs=[vmem] * 2 + [anys] * 7 + [vmem] * 6 + [smem] + [vmem] * 2 + [anys] * 2 + [vmem] * 2,
        out_specs=vmem,
        scratch_shapes=[
            pltpu.VMEM((G * T, r, D), BF16),
            pltpu.VMEM((R, D), BF16),
            pltpu.VMEM((D, (7 if wide else 5) * LANES), BF16),
            pltpu.VMEM((2, 16, LANES) if wide else (2, D, LW), BF16),
            pltpu.VMEM((G,) + extra.shape, F32),
            pltpu.VMEM((S, 2 * LANES), BF16),
            pltpu.VMEM((2, S, LW), BF16),
            pltpu.VMEM((S, LW), F32),
            pltpu.VMEM((N, S, 2 * LANES), BF16),
            pltpu.VMEM((2, S, LANES), BF16),
            pltpu.VMEM((2, S, LANES), F32),
            pltpu.VMEM((2, S, LANES), F32),
            pltpu.VMEM((2, S, LANES), F32),
            pltpu.VMEM((2,) + differential_output_rows.shape, BF16),
            pltpu.VMEM((S, LW), BF16),
            pltpu.VMEM((S, LANES), F32),
            pltpu.VMEM((G + 1, VDIM, LW), F32),
            pltpu.VMEM((G + 1, 1, LW), F32),
            pltpu.VMEM((VDIM, LW), F32),
            pltpu.VMEM((VDIM, LW), F32),
            pltpu.VMEM((2, G, R, LANES), BF16),
            pltpu.VMEM((2, G, R, LANES), BF16),
            pltpu.VMEM((T, r, D), BF16),
            pltpu.VMEM((T, r, D), BF16),
            dma((9,)),
            dma((G,)),
            dma((G * T,)),
            dma((G * T,)),
            dma((G,)),
            dma((G,)),
            dma((N * G,)),
            dma((N * G,)),
            dma((1,)),
            dma((1,)),
            dma((G,)),
            dma((G,)),
            dma((G,)),
            dma((G,)),
            dma((T,)),
            dma((T,)),
        ],
        compiler_params=pltpu.CompilerParams(
            collective_id=0, has_side_effects=True, vmem_limit_bytes=60 * 1024 * 1024
        ),
        name="layer",
    )(
        tokens, row(input_norm_gain), differential_query, differential_key, differential_value,
        linear_query, linear_key, linear_value, linear_output_gate, forget_down_factor.T,
        forget_up_factor, row(forget_bias), extra,
        row(query_norm_gain), row(key_norm_gain), second_map_weight,
        row(differential_norm_gain), row(linear_norm_gain), differential_output_rows,
        linear_output_rows, jnp.asarray(table, BF16), jnp.asarray(pair_level),
    )


def solution(mesh):
    placed = (
        P(("sp", "tp"), None),
        P(),
        P(None, "tp"),
        P(None, "tp"),
        P(None, "tp"),
        P(),
        P(),
        P("tp"),
        P(),
        P(None, "tp"),
        P(None, "tp"),
        P(None, "tp"),
        P(None, "tp"),
        P(),
        P(None, "tp"),
        P("tp"),
        P("sp", "tp"),
        P(),
        P("tp", None),
        P("tp", None),
    )
    return jax.shard_map(
        per_device, mesh=mesh, in_specs=placed, out_specs=P(("sp", "tp"), None), check_vma=False
    )
```

```python
import functools

import jax
import jax.numpy as jnp
import numpy as np
from jax import lax
from jax.experimental import pallas as pl
from jax.experimental.pallas import tpu as pltpu
from jax.sharding import PartitionSpec as P

HEAD = 64
VDIM = 128
RECURRENT_DIM = 64
LANES = 128
RMS_EPS = 1e-06
OUT_SCALE = 0.8
MESH = pl.DeviceIdType.MESH
F32 = jnp.float32
BF16 = jnp.bfloat16


def dot(a, b):
    return jnp.dot(a, b, preferred_element_type=F32)


def dot_t(a, b):
    return lax.dot_general(a, b, (((1,), (1,)), ((), ())), preferred_element_type=F32)


def decay_tables(rows):
    levels = rows.bit_length() - 1
    t = np.arange(rows)[:, None]
    r = np.arange(rows)[None, :]
    parts = []
    for level in range(levels):
        h = 1 << level
        mid = (t // (2 * h)) * 2 * h + h - 1
        upper = (t // h) % 2 == 1
        parts.append(np.where(upper, (r > mid) & (r <= t), (r > t) & (r <= mid)))
    parts.append(r <= t)
    parts.append(r > t)
    pair_level = np.full((rows, rows), -1, np.int32)
    for level in range(levels):
        pair_level[((t ^ r) >> level == 1) & (t > r)] = level
    pair_level[t == r] = levels
    return np.concatenate(parts, 0).astype(np.float32), pair_level, levels


def body(
    cfg,
    tokens, gain, wq, wk, wv, wlq, wlk, wlv, wlg, wdown, up, bias, extra, qgain, kgain, lam,
    dgain, lgain, wo1, wo2, table, pair_level,
    out,
    xbuf, xn, wbuf, wl, ebuf, proj, plin, logs, kv, q2, acc, peak, total, wo, qd, inner, states,
    pre, pref_in, pref_out, obuf, mix, terms, got,
    w_sem, xs_in, xs_tp, x_recv, es, er, kv_send, kv_recv, st_send, st_recv, a_send, a_recv,
    c_send, c_recv, t_send, t_recv,
):
    G, N, T, r, R, S, D, LW, levels = cfg
    sp = lax.axis_index("sp")
    t = lax.axis_index("tp")
    o = lax.div(sp, G)
    i = lax.rem(sp, G)
    wide = LW == LANES
    pairs = LANES // RECURRENT_DIM

    col = pl.multiple_of(i * LANES, LANES)
    lcol = pl.multiple_of(lax.div(i, pairs) * LANES, LANES) if wide else 0
    loads = []
    for n, w in enumerate((wq, wk, wv, wlv, wlg)):
        loads.append(
            pltpu.make_async_copy(
                w.at[:, pl.ds(col, LANES)], wbuf.at[:, pl.ds(n * LANES, LANES)], w_sem.at[n]
            )
        )
    for n, w in enumerate((wlq, wlk)):
        src = w.at[:, pl.ds(lcol, LW)] if wide else w
        dst = wbuf.at[:, pl.ds((5 + n) * LANES, LANES)] if wide else wl.at[n]
        loads.append(pltpu.make_async_copy(src, dst, w_sem.at[5 + n]))
    for copy in loads:
        copy.start()
    wo_loads = [
        pltpu.make_async_copy(w, wo.at[n], w_sem.at[7 + n]) for n, w in enumerate((wo1, wo2))
    ]

    def peer(d):
        return o * G + lax.rem(i + d, G)

    def source(d):
        return lax.rem(i - d + G, G)

    def tpeer(k):
        return lax.rem(t + k, T)

    barrier = pltpu.get_barrier_semaphore()
    for d in range(G):
        for k in range(T):
            if d or k:
                pl.semaphore_signal(
                    barrier, inc=1, device_id=(peer(d), tpeer(k)), device_id_type=MESH
                )

    @pl.when(o > 0)
    def _():
        pl.semaphore_signal(barrier, inc=1, device_id=(sp - G, t), device_id_type=MESH)

    @pl.when(o < N - 1)
    def _():
        pl.semaphore_signal(barrier, inc=1, device_id=(sp + G, t), device_id_type=MESH)

    inside = (o > 0) & (o < N - 1)

    @pl.when(inside)
    def _():
        pl.semaphore_wait(barrier, G * T + 1)

    @pl.when(jnp.logical_not(inside))
    def _():
        pl.semaphore_wait(barrier, G * T if N > 1 else G * T - 1)

    def remote(src, dst, ss, rs, where):
        return pltpu.make_async_remote_copy(
            src_ref=src, dst_ref=dst, send_sem=ss, recv_sem=rs, device_id=where,
            device_id_type=MESH,
        )

    own = i * T + t
    sends = []
    for k in range(1, T):
        sends.append(
            remote(tokens, xbuf.at[own], xs_tp.at[k], x_recv.at[own], (sp, tpeer(k)))
        )
    for d in range(1, G):
        sends.append(remote(tokens, xbuf.at[own], xs_in.at[d], x_recv.at[own], (peer(d), t)))
    for d in range(1, G):
        sends.append(remote(extra, ebuf.at[i], es.at[d], er.at[i], (peer(d), t)))
    for copy in sends:
        copy.start()
    xbuf[own] = tokens[...]
    ebuf[i] = extra[...]

    def arrival(slot):
        remote(
            tokens, xbuf.at[slot], xs_in.at[0], x_recv.at[slot], (peer(1) if G > 1 else sp, tpeer(1))
        ).wait_recv()

    def forward(d):
        j = source(d)
        slot = j * T + t
        arrival(slot)
        for k in range(1, T):
            copy = remote(
                xbuf.at[slot], xbuf.at[slot], xs_tp.at[d * T + k], x_recv.at[slot], (sp, tpeer(k))
            )
            copy.start()
            sends.append(copy)

    lane = lax.broadcasted_iota(jnp.int32, (1, LANES), 1)
    low_half = lane < HEAD

    qg = jnp.concatenate([qgain[...], qgain[...]], axis=1)
    kg = jnp.concatenate([kgain[...], kgain[...]], axis=1)

    def map_norm(values, map_gain):
        sq = values * values
        first = jnp.sum(jnp.where(low_half, sq, 0.0), axis=-1, keepdims=True)
        second = jnp.sum(jnp.where(low_half, 0.0, sq), axis=-1, keepdims=True)
        scale = jnp.where(
            low_half,
            lax.rsqrt(first * (1.0 / HEAD) + RMS_EPS),
            lax.rsqrt(second * (1.0 / HEAD) + RMS_EPS),
        )
        return values * scale * map_gain

    def project(d):
        j = source(d)
        for k in range(1, T):
            arrival(j * T + tpeer(k))
        if d > 0:
            remote(extra, ebuf.at[j], es.at[0], er.at[j], (peer(1), t)).wait_recv()
        for c in range(T):
            x = xbuf[j * T + c].astype(F32)
            ms = jnp.mean(x * x, axis=-1, keepdims=True)
            xn[pl.ds(c * r, r), :] = (x * lax.rsqrt(ms + RMS_EPS) * gain[...]).astype(BF16)
        if d == 0:
            for copy in loads:
                copy.wait()
            for copy in wo_loads:
                copy.start()
        x = xn[...]
        rows = pl.ds(pl.multiple_of(j * R, R), R)
        proj_block = dot(x, wbuf[...]).astype(BF16)
        qn = map_norm(proj_block[:, 0:LANES].astype(F32), qg).astype(BF16) * HEAD ** (-0.5)
        qn = qn.astype(BF16)
        zero = jnp.zeros_like(qn)
        q2[0, rows, :] = jnp.where(low_half, qn, zero)
        q2[1, rows, :] = jnp.where(low_half, zero, qn)
        kn = map_norm(proj_block[:, LANES : 2 * LANES].astype(F32), kg).astype(BF16)
        kv[o, rows, 0:LANES] = kn
        kv[o, rows, LANES : 2 * LANES] = proj_block[:, 2 * LANES : 3 * LANES]
        proj[rows, :] = proj_block[:, 3 * LANES : 5 * LANES]
        if wide:
            mine = lax.div(lane, RECURRENT_DIM) == lax.rem(i, pairs)
            for n in range(2):
                part = proj_block[:, (5 + n) * LANES : (6 + n) * LANES]
                plin[n, rows, :] = jnp.where(mine, part, jnp.zeros_like(part))
        else:
            for n in range(2):
                plin[n, rows, :] = dot(x, wl[n]).astype(BF16)
        low = dot_t(x, wdown[...]).astype(BF16)
        lsl = pl.ds(lcol, LW)
        pre_act = dot(low, up[:, lsl]) + bias[:, lsl]
        log_sig = jnp.minimum(pre_act, 0.0) - jnp.log1p(jnp.exp(-jnp.abs(pre_act)))
        turned = jnp.concatenate([ebuf[j]] + [jnp.zeros((-G % 8, R), F32)] * (G % 8 > 0), axis=0).T
        head_lane = lax.broadcasted_iota(jnp.int32, (1, turned.shape[1]), 1)
        add = jnp.sum(jnp.where(head_lane == i, turned, 0.0), axis=1, keepdims=True)
        logs[rows, :] = log_sig * (1.0 / 16.0) + add

    def kv_copy(slot, j):
        part = kv.at[slot, pl.ds(pl.multiple_of(j * R, R), R)]
        n = slot * G + j
        return remote(part, part, kv_send.at[n], kv_recv.at[n], (sp + G, t))

    def relay(step):
        def one(s, _):
            slot, j = o - s, source(step - s)
            kv_copy(slot, j).wait_recv()

            @pl.when(o < N - 1)
            def _():
                kv_copy(slot, j).start()

            return 0

        lax.fori_loop(jnp.maximum(1, step - G + 1), jnp.minimum(o, step) + 1, one, 0)

    for d in range(G):
        if 0 < d and d + 1 < G:
            forward(d + 1)
        project(d)

        @pl.when(o < N - 1)
        def _():
            kv_copy(o, source(d)).start()

        if d == 0 and G > 1:
            forward(1)
        relay(d)

    level_of = pair_level[...]
    states[...] = jnp.zeros_like(states)
    pre[...] = jnp.zeros_like(pre)

    def chain_block(b, _):
        rows = pl.ds(b * R, R)
        la = logs[rows, :]
        hi = la.astype(BF16)
        lo = (la - hi.astype(F32)).astype(BF16)
        q = plin[0, rows, :].astype(F32) * RECURRENT_DIM ** (-0.5)
        k = plin[1, rows, :].astype(F32)
        v = proj[rows, 0:LANES]
        sums = dot(table[...], hi) + dot(table[...], lo)
        scores = jnp.where(level_of == levels, dot_t(q.astype(BF16), k.astype(BF16)), 0.0)
        for level in range(levels):
            e = jnp.exp(sums[level * R : (level + 1) * R])
            part = dot_t((q * e).astype(BF16), (k * e).astype(BF16))
            scores = scores + jnp.where(level_of == level, part, 0.0)
        inner[rows, :] = dot(scores.astype(BF16), v)
        cum = sums[levels * R : (levels + 1) * R]
        suffix = sums[(levels + 1) * R : (levels + 2) * R]
        qd[rows, :] = (q * jnp.exp(cum)).astype(BF16)
        k_end = (k * jnp.exp(suffix)).astype(BF16)
        last = cum[R - 1 : R, :]
        vt = v.astype(F32).T.astype(BF16)
        states[b + 1] = states[b] * jnp.exp(last) + dot(vt, k_end)
        pre[b + 1] = pre[b] + last
        return 0

    for b in range(G):
        chain_block(b, 0)

    def prefix_copy():
        return remote(
            pref_out.at[...], pref_in.at[...], st_send.at[0], st_recv.at[0], (sp + G, t)
        )

    TQ = min(2 * LANES, S)

    def attend(slot, first):
        k = kv.at[slot]

        def tile(j, _):
            m, start = j // (S // TQ), j % (S // TQ) * TQ
            rows = pl.ds(start, TQ)
            s = dot_t(q2[m, rows, :], k[:, 0:LANES])
            if first:
                u = lax.broadcasted_iota(jnp.int32, (TQ, S), 1)
                tt = lax.broadcasted_iota(jnp.int32, (TQ, S), 0) + start
                s = jnp.where(u <= tt, s, -1e30)
                new = jnp.max(s, axis=-1, keepdims=True)
                p = jnp.exp(s - new)
                total[m, rows, :] = jnp.broadcast_to(
                    jnp.sum(p, axis=-1, keepdims=True), (TQ, LANES)
                )
                acc[m, rows, :] = dot(p.astype(BF16), k[:, LANES : 2 * LANES])
                peak[m, rows, :] = jnp.broadcast_to(new, (TQ, LANES))
            else:
                old = peak[m, rows, :]
                new = jnp.maximum(old, jnp.max(s, axis=-1, keepdims=True))
                p = jnp.exp(s - new[:, 0:1])
                factor = jnp.exp(old - new)
                total[m, rows, :] = total[m, rows, :] * factor + jnp.sum(
                    p, axis=-1, keepdims=True
                )
                acc[m, rows, :] = acc[m, rows, :] * factor + dot(
                    p.astype(BF16), k[:, LANES : 2 * LANES]
                )
                peak[m, rows, :] = new
            return 0

        for j in range(2 * S // TQ):
            tile(j, 0)

    def give(n, ss, rs):
        copies = []
        for d in range(1, G):
            j = lax.rem(i + d, G)
            copies.append(
                remote(obuf.at[n, j], mix.at[n, i], ss.at[d], rs.at[i], (peer(d), t))
            )
        return copies

    def collect(n, ss, rs):
        for d in range(1, G):
            j = source(d)
            remote(obuf.at[n, j], mix.at[n, j], ss.at[0], rs.at[j], (peer(1), t)).wait_recv()

    def chain_finish(b, _):
        rows = pl.ds(b * R, R)
        state = (states[b] + pref_in[...] * jnp.exp(pre[b])).astype(BF16)
        full = inner[rows, :] + dot_t(qd[rows, :], state)
        gate = proj[rows, LANES : 2 * LANES].astype(F32)
        ms = jnp.mean(full * full, axis=-1, keepdims=True)
        gate = gate / (1.0 + jnp.exp(-gate))
        obuf[1, b] = (full * lax.rsqrt(ms + RMS_EPS) * lgain[...] * gate).astype(BF16)
        return 0

    def chain_tail():
        @pl.when(o < N - 1)
        def _():
            pref_out[...] = pref_in[...] * jnp.exp(pre[G]) + states[G]
            prefix_copy().start()

        for b in range(G):
            chain_finish(b, 0)
        for copy in give(1, c_send, c_recv):
            copy.start()
        mix[1, i] = obuf[1, i]

    @pl.when(o == 0)
    def _():
        pref_in[...] = jnp.zeros_like(pref_in)
        chain_tail()

    relay(G)
    attend(o, True)

    def earlier(s, _):
        @pl.when(s > 1)
        def _():
            relay(s + G - 1)

        @pl.when(s == o)
        def _():
            prefix_copy().wait_recv()
            chain_tail()

        attend(o - s, False)
        return 0

    lax.fori_loop(1, o + 1, earlier, 0)
    sends += give(1, c_send, c_recv)

    weight = lam[i]

    def attn_finish(b, _):
        rows = pl.ds(b * R, R)
        diff = acc[0, rows, :] / total[0, rows, :] - weight * (
            acc[1, rows, :] / total[1, rows, :]
        )
        ms = jnp.mean(diff * diff, axis=-1, keepdims=True)
        obuf[0, b] = (diff * lax.rsqrt(ms + RMS_EPS) * dgain[...] * OUT_SCALE).astype(BF16)
        return 0

    for b in range(G):
        attn_finish(b, 0)
    attn_sends = give(0, a_send, a_recv)
    for copy in attn_sends:
        copy.start()
    sends += attn_sends
    mix[0, i] = obuf[0, i]
    for copy in wo_loads:
        copy.wait()
    collect(1, c_send, c_recv)
    chain_mix = jnp.concatenate([mix[1, j] for j in range(G)], axis=1)
    chain_part = dot(chain_mix, wo[1])
    collect(0, a_send, a_recv)
    attn_mix = jnp.concatenate([mix[0, j] for j in range(G)], axis=1)
    term = (dot(attn_mix, wo[0]) + chain_part).astype(BF16)
    for c in range(T):
        terms[c] = term[c * r : (c + 1) * r]
    for k in range(1, T):
        copy = remote(terms.at[tpeer(k)], got.at[t], t_send.at[k], t_recv.at[t], (sp, tpeer(k)))
        copy.start()
        sends.append(copy)
    summed = terms[t].astype(F32)
    for k in range(1, T):
        c = tpeer(k)
        remote(terms.at[c], got.at[c], t_send.at[0], t_recv.at[c], (sp, c)).wait_recv()
        summed = summed + got[c].astype(F32)
    out[...] = summed.astype(BF16)

    for copy in sends:
        copy.wait_send()

    @pl.when(o < N - 1)
    def _():
        prefix_copy().wait_send()

        def drain(s, _):
            for j in range(G):
                kv_copy(s, j).wait_send()
            return 0

        lax.fori_loop(0, o + 1, drain, 0)


def per_device(
    tokens, input_norm_gain, differential_query, differential_key, differential_value,
    query_norm_gain, key_norm_gain, second_map_weight, differential_norm_gain, linear_query,
    linear_key, linear_value, linear_output_gate, forget_down_factor, forget_up_factor,
    forget_bias, extra_shrinkage_exponent, linear_norm_gain, differential_output_rows,
    linear_output_rows,
):
    sp_size, T = lax.axis_size("sp"), lax.axis_size("tp")
    G = second_map_weight.shape[0]
    r, D = tokens.shape
    R = r * T
    N = sp_size // G
    S = G * R
    LW = min(LANES, G * RECURRENT_DIM)
    table, pair_level, levels = decay_tables(R)
    cfg = (G, N, T, r, R, S, D, LW, levels)
    row = lambda a: a.reshape(1, -1)
    extra = extra_shrinkage_exponent.T
    vmem = pl.BlockSpec(memory_space=pltpu.VMEM)
    smem = pl.BlockSpec(memory_space=pltpu.SMEM)
    anys = pl.BlockSpec(memory_space=pl.ANY)
    wide = LW == LANES
    dma = pltpu.SemaphoreType.DMA
    return pl.pallas_call(
        functools.partial(body, cfg),
        out_shape=jax.ShapeDtypeStruct((r, D), BF16),
        in_specs=[vmem] * 2 + [anys] * 7 + [vmem] * 6 + [smem] + [vmem] * 2 + [anys] * 2 + [vmem] * 2,
        out_specs=vmem,
        scratch_shapes=[
            pltpu.VMEM((G * T, r, D), BF16),
            pltpu.VMEM((R, D), BF16),
            pltpu.VMEM((D, (7 if wide else 5) * LANES), BF16),
            pltpu.VMEM((2, 16, LANES) if wide else (2, D, LW), BF16),
            pltpu.VMEM((G,) + extra.shape, F32),
            pltpu.VMEM((S, 2 * LANES), BF16),
            pltpu.VMEM((2, S, LW), BF16),
            pltpu.VMEM((S, LW), F32),
            pltpu.VMEM((N, S, 2 * LANES), BF16),
            pltpu.VMEM((2, S, LANES), BF16),
            pltpu.VMEM((2, S, LANES), F32),
            pltpu.VMEM((2, S, LANES), F32),
            pltpu.VMEM((2, S, LANES), F32),
            pltpu.VMEM((2,) + differential_output_rows.shape, BF16),
            pltpu.VMEM((S, LW), BF16),
            pltpu.VMEM((S, LANES), F32),
            pltpu.VMEM((G + 1, VDIM, LW), F32),
            pltpu.VMEM((G + 1, 1, LW), F32),
            pltpu.VMEM((VDIM, LW), F32),
            pltpu.VMEM((VDIM, LW), F32),
            pltpu.VMEM((2, G, R, LANES), BF16),
            pltpu.VMEM((2, G, R, LANES), BF16),
            pltpu.VMEM((T, r, D), BF16),
            pltpu.VMEM((T, r, D), BF16),
            dma((9,)),
            dma((G,)),
            dma((G * T,)),
            dma((G * T,)),
            dma((G,)),
            dma((G,)),
            dma((N * G,)),
            dma((N * G,)),
            dma((1,)),
            dma((1,)),
            dma((G,)),
            dma((G,)),
            dma((G,)),
            dma((G,)),
            dma((T,)),
            dma((T,)),
        ],
        compiler_params=pltpu.CompilerParams(
            collective_id=0, has_side_effects=True, vmem_limit_bytes=60 * 1024 * 1024
        ),
        name="layer",
    )(
        tokens, row(input_norm_gain), differential_query, differential_key, differential_value,
        linear_query, linear_key, linear_value, linear_output_gate, forget_down_factor.T,
        forget_up_factor, row(forget_bias), extra,
        row(query_norm_gain), row(key_norm_gain), second_map_weight,
        row(differential_norm_gain), row(linear_norm_gain), differential_output_rows,
        linear_output_rows, jnp.asarray(table, BF16), jnp.asarray(pair_level),
    )


def solution(mesh):
    placed = (
        P(("sp", "tp"), None),
        P(),
        P(None, "tp"),
        P(None, "tp"),
        P(None, "tp"),
        P(),
        P(),
        P("tp"),
        P(),
        P(None, "tp"),
        P(None, "tp"),
        P(None, "tp"),
        P(None, "tp"),
        P(),
        P(None, "tp"),
        P("tp"),
        P("sp", "tp"),
        P(),
        P("tp", None),
        P("tp", None),
    )
    return jax.shard_map(
        per_device, mesh=mesh, in_specs=placed, out_specs=P(("sp", "tp"), None), check_vma=False
    )
```
